32 devices in a mesh: ep: 8 (over z, x), tp: 4 (over y, core).
Axes of the slice: x: 2, y: 2, z: 4, core: 2. Of those that a mesh axis runs over, the one named last changes fastest.
Arguments:
- residual: bfloat16 [256, 2048], P('ep'), may hold values from -6 to 6
- routes: int32 [256, 4], P('ep'), may hold values from 0 to 7, as said below
- lengths: int32 [256], P('ep'), may hold values from 1 to 512, as said below
- key_cache: bfloat16 [256, 512, 4, 128], P('ep', None, 'tp'), may hold values from -6 to 6
- value_cache: bfloat16 [256, 512, 4, 128], P('ep', None, 'tp'), may hold values from -6 to 6
- mix_gain: float32 [2048], replicated, may hold values from 0.1 to 1.9
- w_query: bfloat16 [2048, 2048], P(None, 'tp'), may hold values from -0.125 to 0.125
- w_out: bfloat16 [2048, 2048], P('tp'), may hold values from -0.375 to 0.375
- head_bias: float32 [16], P('tp'), may hold values from -7 to -1
- moe_gain: float32 [2048], replicated, may hold values from 0.1 to 1.9
- w_group: bfloat16 [2048, 1], replicated, may hold values from -0.02734375 to 0.02734375
- w_expert: bfloat16 [2048, 8], replicated, may hold values from -0.02734375 to 0.02734375
- expert_gate: bfloat16 [8, 2048, 1024], P('ep', None, 'tp'), may hold values from -0.125 to 0.125
- expert_up: bfloat16 [8, 2048, 1024], P('ep', None, 'tp'), may hold values from -0.125 to 0.125
- expert_down: bfloat16 [8, 1024, 2048], P('ep', 'tp'), may hold values from -3 to 3
Outputs:
- layer_out: bfloat16 [256, 2048], P('ep', 'tp')
The draws below stay inside these ranges and needn't reach their ends.
Inputs may be any that keep to these rules, and one draw needn't show every extreme that they name: `routes`: each row names 4 different experts, all in one group of 8 consecutive experts. Within the rows of one device (aligned blocks of 32 rows) no expert is named more than 16 times, and some expert is named exactly 16 times in every block. `lengths`: some sequence has 512 cached positions in every draw.
All inputs are finite; a program needn't handle non-finite values.
Results may differ from the reference program's by a relative error of at most 0.02.
Values may be sent and summed in bfloat16 or wider, within the bound.
A program may use at most 64 MiB of HBM per device.

```python
import jax
import jax.numpy as jnp
from jax import lax

D = 2048
HEADS = 16
HEAD_SIZE = 128
KV_HEADS = 4
FF = 1024
GROUP_SIZE = 8
TOPK = 4
SEQ_DEV = 32
CACHE = 512
SEQS = 256
EXPERTS = 8
GROUPS = 1
GROUP_MOST = 32
CAPACITY = 16
N_TP = 4


def draw_routes(key, part):
    streams = jax.random.split(jax.random.fold_in(key, 11), 4)
    blocks = SEQS // SEQ_DEV
    groups = EXPERTS // GROUP_SIZE
    warmth = jax.random.randint(streams[0], (1, groups), 0, 4)
    jitter = jax.random.randint(streams[1], (blocks, groups), 0, 4)
    ranking = (warmth + jitter) * groups + jnp.arange(groups, dtype=jnp.int32)[None, :]
    ordering = jnp.argsort(-ranking, axis=1)
    shuffle = jax.random.randint(streams[2], (blocks, SEQ_DEV), 0, SEQ_DEV) * SEQ_DEV + jnp.arange(SEQ_DEV, dtype=jnp.int32)[None, :]
    ranked = jnp.argsort(jnp.argsort(shuffle, axis=1), axis=1)
    group_id = jnp.take_along_axis(ordering, ranked // GROUP_MOST, axis=1)
    within = ranked % GROUP_MOST
    rotate = jax.random.randint(streams[3], (blocks, groups), 0, GROUP_SIZE)
    offset = jnp.take_along_axis(rotate, group_id, axis=1)
    member = (offset[:, :, None] + within[:, :, None] * TOPK + jnp.arange(TOPK, dtype=jnp.int32)[None, None, :]) % GROUP_SIZE
    return (group_id[:, :, None] * GROUP_SIZE + member).reshape(SEQS, TOPK).astype(jnp.int32)


def draw_lengths(key, part):
    streams = jax.random.split(jax.random.fold_in(key, 23), 3)
    blocks = SEQS // SEQ_DEV
    levels = jax.random.randint(streams[0], (blocks, 1), 1, 9)
    drawn = jax.random.randint(streams[1], (blocks, SEQ_DEV), 1, CACHE + 1)
    scaled = (1 + (drawn - 1) * levels // 8).reshape(SEQS)
    chosen = jax.random.randint(streams[2], (), 0, SEQS)
    filled = jnp.where(jnp.arange(SEQS, dtype=jnp.int32) == chosen, CACHE, scaled)
    return filled.astype(jnp.int32)


def shard_levels(key, extent, cuts, least, high):
    gain, own = 1.0, jax.random.fold_in(key, 6)
    for position, blocks in cuts:
        steps = jnp.exp(jax.random.uniform(jax.random.fold_in(own, position), (blocks,), jnp.float32, least / len(cuts), high / len(cuts)))
        gain = gain * jnp.repeat(steps, extent[position] // blocks).reshape([-1 if axis == position else 1 for axis in range(len(extent))])
    return gain


def noise(stream_key, dims, deviation, bound, shards=(), kind=jnp.bfloat16):
    level = shard_levels(stream_key, dims, shards, -0.22, 0.18) if shards else 1.0
    array = jax.random.normal(stream_key, dims, jnp.float32) * deviation * level
    return jnp.minimum(jnp.maximum(array, -bound), bound).astype(kind)


def setup_inputs(seed: int = 0) -> dict:
    seeds = jax.random.split(jax.random.key(seed), 16)
    return {
        "residual": noise(seeds[0], (SEQS, D), 1.0, 6.0, ((0, 8),)),
        "routes": draw_routes(jax.random.fold_in(seeds[15], 71), 0),
        "lengths": draw_lengths(jax.random.fold_in(seeds[15], 71), 0),
        "key_cache": noise(seeds[3], (SEQS, CACHE, KV_HEADS, HEAD_SIZE), 1.0, 6.0, ((0, 8), (2, 4))),
        "value_cache": noise(seeds[4], (SEQS, CACHE, KV_HEADS, HEAD_SIZE), 1.0, 6.0, ((0, 8), (2, 4))),
        "mix_gain": jnp.clip(1.0 + 0.18 * jax.random.normal(seeds[5], (D,), jnp.float32), 0.1, 1.9),
        "w_query": noise(seeds[6], (D, HEADS * HEAD_SIZE), D ** -0.5, 0.125, ((1, 4),)),
        "w_out": noise(seeds[7], (HEADS * HEAD_SIZE, D), (HEADS * HEAD_SIZE // 9) ** -0.5, 0.375, ((0, 4),)),
        "head_bias": jnp.clip(-7.0 + 6.0 * jax.random.uniform(seeds[8], (HEADS,), jnp.float32) ** shard_levels(seeds[8], (HEADS,), ((0, 4),), -0.2, 0.2), -7.0, -1.0),
        "moe_gain": jnp.clip(1.0 + 0.18 * jax.random.normal(seeds[9], (D,), jnp.float32), 0.1, 1.9),
        "w_group": noise(seeds[10], (D, GROUPS), (25 * D) ** -0.5, 0.02734375),
        "w_expert": noise(seeds[11], (D, EXPERTS), (25 * D) ** -0.5, 0.02734375),
        "expert_gate": noise(seeds[12], (EXPERTS, D, FF), D ** -0.5, 0.125, ((0, 8), (2, 4))),
        "expert_up": noise(seeds[13], (EXPERTS, D, FF), D ** -0.5, 0.125, ((0, 8), (2, 4))),
        "expert_down": noise(seeds[14], (EXPERTS, FF, D), (max(1, FF // 256)) ** -0.5, 3.0, ((0, 8), (1, 4))),
    }


EPSILON = 1e-06

def rms_scale(tokens, gains):
    values = tokens.astype(jnp.float32)
    inverse = lax.rsqrt(lax.optimization_barrier(jnp.mean(values * values, axis=-1, keepdims=True)) + EPSILON)
    return (values * inverse * gains.astype(jnp.float32)).astype(jnp.bfloat16)

def rounded(values):
    return lax.optimization_barrier(values.astype(jnp.bfloat16)).astype(jnp.float32)

def place_rows(buffer, target, source):
    return buffer.at[target].set(source)

def reference(residual, routes, lengths, key_cache, value_cache, mix_gain, w_query, w_out, head_bias, moe_gain, w_group, w_expert, expert_gate, expert_up, expert_down):
    tokens = residual.shape[0]
    normed = rms_scale(residual, mix_gain)
    queries = jnp.dot(normed, w_query, preferred_element_type=jnp.float32).astype(jnp.bfloat16)
    key_heads = key_cache.shape[2]
    head_size = key_cache.shape[3]
    per_key = HEADS // key_heads
    bias_grid = head_bias.astype(jnp.float32).reshape(key_heads, per_key)
    grouped = queries.reshape(tokens, key_heads, per_key, head_size)

    def stick_one(item):
        query_rows, key_rows, value_rows, length = item
        scores = jnp.einsum('kgd,lkd->kgl', query_rows.astype(jnp.float32), key_rows.astype(jnp.float32)) * head_size ** (-0.5)
        scores = scores + bias_grid[:, :, None]
        inside = lax.broadcasted_iota(jnp.int32, scores.shape, 2) < length
        remain = jnp.where(inside, jax.nn.log_sigmoid(-scores), 0.0)
        later_sum = lax.cumsum(remain, axis=2, reverse=True) - remain
        weights = jnp.where(inside, jnp.exp(jax.nn.log_sigmoid(scores) + later_sum), 0.0)
        mixture = jnp.einsum('kgl,lkd->kgd', rounded(weights), value_rows.astype(jnp.float32))
        return mixture.astype(jnp.bfloat16)
    attended = lax.map(stick_one, (grouped, key_cache, value_cache, lengths)).reshape(tokens, HEADS * head_size)
    block = HEADS * head_size // N_TP
    head_part = jnp.einsum('tpc,pcd->ptd', attended.reshape(tokens, N_TP, block).astype(jnp.float32), w_out.reshape(N_TP, block, D).astype(jnp.float32))
    attn_out = lax.optimization_barrier(jnp.sum(rounded(head_part), axis=0)).astype(jnp.bfloat16)
    mid = (residual.astype(jnp.float32) + attn_out.astype(jnp.float32)).astype(jnp.bfloat16)
    hidden_in = rms_scale(mid, moe_gain)
    group_prob = jax.nn.softmax(jnp.dot(hidden_in, w_group, preferred_element_type=jnp.float32), axis=-1)
    expert_logit = jnp.dot(hidden_in, w_expert, preferred_element_type=jnp.float32)
    picked = jnp.take_along_axis(expert_logit, routes, axis=1)
    top_prob = jnp.take_along_axis(group_prob, routes[:, :1] // GROUP_SIZE, axis=1)
    share = jax.nn.softmax(picked, axis=1) * top_prob
    expert_count = w_expert.shape[1]
    blocks = tokens // SEQ_DEV
    block_routes = routes.reshape(blocks, SEQ_DEV * TOPK)
    onehot = (block_routes[:, :, None] == jnp.arange(expert_count, dtype=jnp.int32)[None, None, :]).astype(jnp.int32)
    earlier = jnp.cumsum(onehot, axis=1, dtype=jnp.int32) - onehot
    slot = lax.optimization_barrier(jnp.sum(earlier * onehot, axis=2, dtype=jnp.int32)).astype(jnp.int32)
    target = (block_routes * CAPACITY + slot).astype(jnp.int32)
    source_rows = jnp.repeat(hidden_in.reshape(blocks, SEQ_DEV, D), TOPK, axis=1)
    buffer = jnp.zeros((blocks, expert_count * CAPACITY, D), jnp.bfloat16)
    buffer = jax.vmap(place_rows)(buffer, target, source_rows)
    arranged = buffer.reshape(blocks, expert_count, CAPACITY, D).transpose(1, 0, 2, 3).reshape(expert_count, blocks * CAPACITY, D)
    slab = FF // N_TP

    def run_expert(item):
        batch_rows, gate_weight, up_weight, down_weight = item
        gate = jnp.dot(batch_rows, gate_weight, preferred_element_type=jnp.float32)
        upward = jnp.dot(batch_rows, up_weight, preferred_element_type=jnp.float32)
        active = (jax.nn.silu(gate) * upward).astype(jnp.bfloat16)
        parts = jnp.einsum('rpf,pfd->prd', active.reshape(-1, N_TP, slab).astype(jnp.float32), down_weight.reshape(N_TP, slab, D).astype(jnp.float32))
        return lax.optimization_barrier(jnp.sum(rounded(parts), axis=0)).astype(jnp.bfloat16)
    outputs = lax.map(run_expert, (arranged, expert_gate, expert_up, expert_down))
    outputs = outputs.reshape(expert_count, blocks, CAPACITY, D)
    block_index = jnp.arange(tokens * TOPK, dtype=jnp.int32) // (SEQ_DEV * TOPK)
    pair_out = outputs[routes.reshape(-1), block_index, slot.reshape(-1)].reshape(tokens, TOPK, D)
    moe = lax.optimization_barrier(jnp.sum(share[:, :, None] * pair_out.astype(jnp.float32), axis=1))
    return (mid.astype(jnp.float32) + moe).astype(jnp.bfloat16)
```

```python
import functools

import jax
import jax.numpy as jnp
from jax import lax
from jax.experimental import pallas as pl
from jax.experimental.pallas import tpu as pltpu
from jax.sharding import PartitionSpec as P

GROUP_SIZE = 8
TOPK = 4
EPSILON = 1e-06
MESH = pl.DeviceIdType.MESH
BF = jnp.bfloat16
F32 = jnp.float32
KEY_CHUNKS = 4
NT = (((1,), (1,)), ((), ()))
TN = (((0,), (0,)), ((), ()))


def split3(values):
    first = values.astype(BF)
    rest = values - first.astype(F32)
    second = rest.astype(BF)
    third = (rest - second.astype(F32)).astype(BF)
    return first, second, third


def remote(src, dst, send, recv, device):
    return pltpu.make_async_remote_copy(
        src_ref=src, dst_ref=dst, send_sem=send, recv_sem=recv,
        device_id=device, device_id_type=MESH,
    )


def kernel(
    n_ep, n_tp, capacity,
    lens_ref, bias_ref, routes_ref, wexp_ref, wgrp_ref,
    mixg_hbm, moeg_hbm, res_hbm, wq_hbm, key_hbm, value_hbm, wo_hbm, wg_hbm, wu_hbm, wd_hbm,
    out_ref,
    mixg, moeg, res, wq, keys, values, wo, wg, wu, wd,
    qs, scores, sticks, att, head_send, head_recv, mid_all, slots, full,
    part_send, part_recv, pair_send, pair_recv, ret_send, ret_recv,
    small_sem, weight_sem, key_sem, value_sem,
    head_ss, head_rs, mid_ss, mid_rs, disp_ss, disp_rs,
    core_ss, core_rs, cross_ss, cross_rs, fwd_ss, fwd_rs,
    part_ss, part_rs, pair_ss, pair_rs, ret_ss, ret_rs,
):
    ep = lax.axis_index("ep")
    tp = lax.axis_index("tp")
    near = tp + 1 - 2 * (tp % 2)
    far = (tp + 2) % n_tp
    diag = (near + 2) % n_tp
    seqs, width = res.shape
    own = width // n_tp
    heads = bias_ref.shape[0] // seqs
    size = keys.shape[2]
    experts = wexp_ref.shape[0]

    def ep_peer(d):
        return lax.rem(ep + d, n_ep)

    def ep_source(d):
        return lax.rem(ep + n_ep - d, n_ep)

    loads = [
        pltpu.make_async_copy(src, dst, small_sem.at[i])
        for i, (src, dst) in enumerate(((res_hbm, res), (mixg_hbm, mixg), (moeg_hbm, moeg)))
    ]
    weights = [
        pltpu.make_async_copy(src, dst, weight_sem.at[i])
        for i, (src, dst) in enumerate(
            ((wq_hbm, wq), (wo_hbm, wo), (wg_hbm, wg), (wu_hbm, wu), (wd_hbm, wd))
        )
    ]
    step = seqs // KEY_CHUNKS
    key_loads = []
    value_loads = []
    for c in range(KEY_CHUNKS):
        rows = pl.ds(c * step, step)
        key_loads.append(pltpu.make_async_copy(key_hbm.at[rows], keys.at[rows], key_sem.at[c]))
        value_loads.append(
            pltpu.make_async_copy(value_hbm.at[rows], values.at[rows], value_sem.at[c])
        )
    for copy in loads + weights[:1] + key_loads + value_loads + weights[1:]:
        copy.start()

    barrier = pltpu.get_barrier_semaphore()
    for d in range(1, n_tp):
        pl.semaphore_signal(
            barrier, inc=1, device_id={"tp": lax.rem(tp + d, n_tp)}, device_id_type=MESH
        )

    @pl.loop(1, n_ep)
    def _(d):
        pl.semaphore_signal(barrier, inc=1, device_id={"ep": ep_peer(d)}, device_id_type=MESH)

    for copy in loads:
        copy.wait()
    tokens = res[...].astype(F32)
    inverse = lax.rsqrt(jnp.sum(tokens * tokens, axis=1, keepdims=True) / width + EPSILON)
    normed = (tokens * inverse * mixg[...]).astype(BF)
    weights[0].wait()
    queries = jnp.dot(normed, wq[...], preferred_element_type=F32).astype(BF).astype(F32)
    for h in range(heads):
        qs[pl.ds(h, seqs, stride=heads), :] = queries[:, h * size:(h + 1) * size]
    per = 8 // heads
    row_of = lax.broadcasted_iota(jnp.int32, (8, 1), 0)
    for t in range(0, seqs, per):
        if t % step == 0:
            key_loads[t // step].wait()
        rows = qs[t * heads:t * heads + 8, :].astype(BF)
        total = None
        for j in range(per):
            term = lax.dot_general(rows, keys[t + j], NT, preferred_element_type=F32)
            total = term if total is None else jnp.where(row_of < j * heads, total, term)
        scores[t * heads:t * heads + 8, :] = total
    length = keys.shape[1]
    z = scores[...] * size ** (-0.5) + bias_ref[...]
    inside = lax.broadcasted_iota(jnp.int32, z.shape, 1) < lens_ref[...]
    low = jnp.log1p(jnp.exp(-jnp.abs(z)))
    remain = jnp.where(inside, -(jnp.maximum(z, 0.0) + low), 0.0)
    after = (
        lax.broadcasted_iota(jnp.int32, (length, length), 0)
        > lax.broadcasted_iota(jnp.int32, (length, length), 1)
    ).astype(F32).astype(BF)
    later = None
    for term in split3(remain):
        value = jnp.dot(term, after, preferred_element_type=F32)
        later = value if later is None else later + value
    sticks[...] = jnp.where(inside, jnp.exp(jnp.minimum(z, 0.0) - low + later), 0.0)
    for t in range(0, seqs, per):
        if t % step == 0:
            value_loads[t // step].wait()
        rows = sticks[t * heads:t * heads + 8, :].astype(BF)
        total = None
        for j in range(per):
            term = jnp.dot(rows, values[t + j], preferred_element_type=F32)
            total = term if total is None else jnp.where(row_of < j * heads, total, term)
        att[t * heads:t * heads + 8, :] = total
    attended = jnp.concatenate(
        [att[pl.ds(h, seqs, stride=heads), :].astype(BF) for h in range(heads)], axis=1
    )
    weights[1].wait()
    for p in range(n_tp):
        head_send[p] = jnp.dot(
            attended, wo[:, p * own:(p + 1) * own], preferred_element_type=F32
        ).astype(BF)

    pl.semaphore_wait(barrier, n_tp - 1 + n_ep - 1)
    head_copies = []
    for d in range(1, n_tp):
        peer = lax.rem(tp + d, n_tp)
        head_copies.append(
            remote(head_send.at[peer], head_recv.at[d], head_ss.at[d], head_rs.at[d], {"tp": peer})
        )
        head_copies[-1].start()

    routes = routes_ref[...]
    expert_row = lax.broadcasted_iota(jnp.int32, (experts, seqs), 0)
    chosen = jnp.zeros((experts, seqs), F32)
    for k in range(TOPK):
        chosen = chosen + jnp.where(routes[k:k + 1, :] == expert_row, 1.0, 0.0)
    before = (
        lax.broadcasted_iota(jnp.int32, (seqs, seqs), 0)
        < lax.broadcasted_iota(jnp.int32, (seqs, seqs), 1)
    ).astype(F32).astype(BF)
    earlier = jnp.dot(chosen.astype(BF), before, preferred_element_type=F32)
    slot_of = jnp.where(chosen > 0.5, earlier, -1.0)
    slot_row = lax.broadcasted_iota(jnp.int32, (experts, capacity, seqs), 1).astype(F32)
    place = jnp.where(
        jnp.broadcast_to(slot_of[:, None, :], slot_row.shape) == slot_row, 1.0, 0.0
    ).reshape(experts * capacity, seqs)

    attn = head_send[tp].astype(F32)
    for copy in head_copies:
        copy.wait_recv()
    for d in range(1, n_tp):
        attn = attn + head_recv[d].astype(F32)
    own_columns = pl.ds(pl.multiple_of(tp * own, own), own)
    mid_own = (
        res[:, own_columns].astype(F32) + attn.astype(BF).astype(F32)
    ).astype(BF)
    routed = jnp.dot(place.astype(BF), mid_own, preferred_element_type=F32).astype(BF)
    slots[...] = routed.reshape(experts, capacity, own)
    mid_all[tp] = mid_own

    def dispatch(d):
        return remote(
            slots.at[ep_peer(d)], full.at[tp, ep], disp_ss.at[d], disp_rs.at[d],
            {"ep": ep_peer(d)},
        )

    @pl.loop(1, n_ep)
    def _(d):
        dispatch(d).start()

    full[tp, ep] = slots[ep]
    mid_copies = []
    for d in range(1, n_tp):
        peer = lax.rem(tp + d, n_tp)
        mid_copies.append(
            remote(mid_all.at[tp], mid_all.at[tp], mid_ss.at[d], mid_rs.at[d], {"tp": peer})
        )

    def to_core(d):
        at = (tp, ep_source(d))
        return remote(full.at[at], full.at[at], core_ss.at[d], core_rs.at[d], {"tp": near})

    def to_far(d):
        at = (tp, ep_source(d))
        return remote(full.at[at], full.at[at], cross_ss.at[d], cross_rs.at[d], {"tp": far})

    def onward(d):
        at = (far, ep_source(d))
        return remote(full.at[at], full.at[at], fwd_ss.at[d], fwd_rs.at[d], {"tp": near})

    to_far(0).start()
    to_core(0).start()

    @pl.loop(1, n_ep)
    def _(d):
        dispatch(d).wait_recv()
        to_far(d).start()
        to_core(d).start()

    for copy in mid_copies:
        copy.start()

    @pl.loop(0, n_ep)
    def _(d):
        to_far(d).wait_recv()
        onward(d).start()

    for copy in weights[2:]:
        copy.wait()

    @pl.loop(0, n_ep)
    def _(d):
        to_core(d).wait_recv()

    @pl.loop(0, n_ep)
    def _(d):
        onward(d).wait_recv()

    rows = n_ep * capacity
    squares = jnp.zeros((rows, 1), F32)
    for p in range(n_tp):
        block = full[p].reshape(rows, own).astype(F32)
        squares = squares + jnp.sum(block * block, axis=1, keepdims=True)
    inverse = lax.rsqrt(squares / width + EPSILON)
    gate = None
    for p in range(n_tp):
        columns = slice(p * own, (p + 1) * own)
        block = full[p].reshape(rows, own).astype(F32)
        hidden = (block * inverse * moeg[:, columns]).astype(BF)
        gate_term = jnp.dot(hidden, wg[columns, :], preferred_element_type=F32)
        up_term = jnp.dot(hidden, wu[columns, :], preferred_element_type=F32)
        gate = gate_term if gate is None else gate + gate_term
        upward = up_term if p == 0 else upward + up_term
    active = (gate / (1.0 + jnp.exp(-gate)) * upward).astype(BF)

    def partial_of(p):
        columns = pl.ds(pl.multiple_of(p * own, own), own)
        value = jnp.dot(active, wd[:, columns], preferred_element_type=F32)
        return value.astype(BF).reshape(n_ep, capacity, own)

    part_copies = []
    for i, peer in enumerate((diag, near)):
        part_send[i] = partial_of(peer)
        part_copies.append(
            remote(part_send.at[i], part_recv.at[i], part_ss.at[i], part_rs.at[i], {"tp": near})
        )
        part_copies[-1].start()
    far_part = partial_of(far).astype(F32)
    part_copies[0].wait_recv()
    pair_send[...] = (far_part + part_recv[0].astype(F32)).astype(BF)

    def pair(d):
        at = ep_source(d)
        return remote(
            pair_send.at[at], pair_recv.at[at], pair_ss.at[d], pair_rs.at[d], {"tp": far}
        )

    @pl.loop(1, n_ep)
    def _(d):
        pair(d).start()

    pair(0).start()
    own_part = partial_of(tp).astype(F32)
    part_copies[1].wait_recv()
    ret_send[...] = own_part + part_recv[1].astype(F32)

    def giving(d):
        at = ep_source(d)
        return remote(slots.at[at], ret_recv.at[ep], ret_ss.at[d], ret_rs.at[d], {"ep": at})

    @pl.loop(1, n_ep)
    def _(d):
        dispatch(d).wait_send()

    @pl.loop(1, n_ep)
    def _(d):
        at = ep_source(d)
        pair(d).wait_recv()
        slots[at] = (ret_send[at] + pair_recv[at].astype(F32)).astype(BF)
        giving(d).start()

    pair(0).wait_recv()
    ret_recv[ep] = (ret_send[ep] + pair_recv[ep].astype(F32)).astype(BF)

    for copy in mid_copies:
        copy.wait_recv()
    squares = jnp.zeros((seqs, 1), F32)
    for p in range(n_tp):
        block = mid_all[p].astype(F32)
        squares = squares + jnp.sum(block * block, axis=1, keepdims=True)
    inverse = lax.rsqrt(squares / width + EPSILON)
    logit = jnp.zeros((experts, seqs), F32)
    group_logit = jnp.zeros((wgrp_ref.shape[0], seqs), F32)
    for p in range(n_tp):
        columns = slice(p * own, (p + 1) * own)
        hidden = (mid_all[p].astype(F32) * inverse * moeg[:, columns]).astype(BF)
        logit = logit + lax.dot_general(
            wexp_ref[:, columns], hidden, NT, preferred_element_type=F32
        )
        group_logit = group_logit + lax.dot_general(
            wgrp_ref[:, columns], hidden, NT, preferred_element_type=F32
        )
    group_exp = jnp.exp(group_logit - jnp.max(group_logit, axis=0, keepdims=True))
    group_prob = group_exp / jnp.sum(group_exp, axis=0, keepdims=True)
    group_row = lax.broadcasted_iota(jnp.int32, group_prob.shape, 0)
    group_of = jnp.zeros((1, seqs), jnp.int32) + lax.shift_right_logical(
        routes[0:1, :], jnp.full((1, seqs), GROUP_SIZE.bit_length() - 1, jnp.int32)
    )
    top_prob = jnp.sum(jnp.where(group_of == group_row, group_prob, 0.0), axis=0, keepdims=True)
    peak = jnp.max(jnp.where(chosen > 0.5, logit, -jnp.inf), axis=0, keepdims=True)
    raised = jnp.where(chosen > 0.5, jnp.exp(jnp.minimum(logit - peak, 0.0)), 0.0)
    share = raised / jnp.sum(raised, axis=0, keepdims=True) * top_prob
    combine = place * jnp.broadcast_to(share[:, None, :], slot_row.shape).reshape(place.shape)

    @pl.loop(1, n_ep)
    def _(d):
        remote(
            slots.at[ep], ret_recv.at[ep_peer(d)], ret_ss.at[d], ret_rs.at[d], {"ep": ep_source(d)}
        ).wait_recv()

    returned = ret_recv[...].reshape(experts * capacity, own)
    moe = None
    for term in split3(combine):
        value = lax.dot_general(term, returned, TN, preferred_element_type=F32)
        moe = value if moe is None else moe + value
    out_ref[...] = (mid_all[tp].astype(F32) + moe).astype(BF)

    for copy in head_copies + mid_copies + part_copies:
        copy.wait_send()

    @pl.loop(0, n_ep)
    def _(d):
        to_core(d).wait_send()
        to_far(d).wait_send()
        onward(d).wait_send()
        pair(d).wait_send()

    @pl.loop(1, n_ep)
    def _(d):
        giving(d).wait_send()


def per_device(
    n_ep, n_tp,
    residual, routes, lengths, key_cache, value_cache, mix_gain, w_query, w_out, head_bias,
    moe_gain, w_group, w_expert, expert_gate, expert_up, expert_down,
):
    seqs, width = residual.shape
    length, size = key_cache.shape[1], key_cache.shape[3]
    heads = head_bias.shape[0]
    experts, groups = w_expert.shape[1], w_group.shape[1]
    assert key_cache.shape[2] == 1 and expert_gate.shape[0] == 1 and n_tp == 4
    assert experts == n_ep
    own = width // n_tp
    units = expert_gate.shape[2]
    most = min(seqs, max(4, 2 * seqs // groups)) * TOPK // GROUP_SIZE
    capacity = -(-most // 16) * 16
    rows = seqs * heads
    vmem = pl.BlockSpec(memory_space=pltpu.VMEM)
    hbm = pl.BlockSpec(memory_space=pltpu.HBM)
    dma = pltpu.SemaphoreType.DMA
    return pl.pallas_call(
        functools.partial(kernel, n_ep, n_tp, capacity),
        out_shape=jax.ShapeDtypeStruct((seqs, own), BF),
        in_specs=[vmem] * 5 + [hbm] * 10,
        out_specs=vmem,
        scratch_shapes=[
            pltpu.VMEM((1, width), F32),
            pltpu.VMEM((1, width), F32),
            pltpu.VMEM((seqs, width), BF),
            pltpu.VMEM(w_query.shape, BF),
            pltpu.VMEM((seqs, length, size), BF),
            pltpu.VMEM((seqs, length, size), BF),
            pltpu.VMEM(w_out.shape, BF),
            pltpu.VMEM((width, units), BF),
            pltpu.VMEM((width, units), BF),
            pltpu.VMEM((units, width), BF),
            pltpu.VMEM((rows, size), F32),
            pltpu.VMEM((rows, length), F32),
            pltpu.VMEM((rows, length), F32),
            pltpu.VMEM((rows, size), F32),
            pltpu.VMEM((n_tp, seqs, own), BF),
            pltpu.VMEM((n_tp, seqs, own), BF),
            pltpu.VMEM((n_tp, seqs, own), BF),
            pltpu.VMEM((n_ep, capacity, own), BF),
            pltpu.VMEM((n_tp, n_ep, capacity, own), BF),
            pltpu.VMEM((2, n_ep, capacity, own), BF),
            pltpu.VMEM((2, n_ep, capacity, own), BF),
            pltpu.VMEM((n_ep, capacity, own), BF),
            pltpu.VMEM((n_ep, capacity, own), BF),
            pltpu.VMEM((n_ep, capacity, own), F32),
            pltpu.VMEM((n_ep, capacity, own), BF),
            dma((3,)), dma((5,)), dma((KEY_CHUNKS,)), dma((KEY_CHUNKS,)),
            dma((n_tp,)), dma((n_tp,)), dma((n_tp,)), dma((n_tp,)),
            dma((n_ep,)), dma((n_ep,)),
            dma((n_ep,)), dma((n_ep,)), dma((n_ep,)), dma((n_ep,)), dma((n_ep,)), dma((n_ep,)),
            dma((2,)), dma((2,)), dma((n_ep,)), dma((n_ep,)), dma((n_ep,)), dma((n_ep,)),
        ],
        compiler_params=pltpu.CompilerParams(
            collective_id=0, has_side_effects=True, vmem_limit_bytes=60 * 1024 * 1024
        ),
        name="decode_step",
    )(
        jnp.repeat(lengths, heads)[:, None],
        jnp.tile(head_bias, seqs)[:, None],
        routes.T,
        w_expert.T,
        w_group.T,
        mix_gain.reshape(1, width),
        moe_gain.reshape(1, width),
        residual,
        w_query,
        key_cache.reshape(seqs, length, size),
        value_cache.reshape(seqs, length, size),
        w_out,
        expert_gate.reshape(width, units),
        expert_up.reshape(width, units),
        expert_down.reshape(units, width),
    )


def solution(mesh):
    in_specs = (
        P("ep", None),
        P("ep", None),
        P("ep"),
        P("ep", None, "tp", None),
        P("ep", None, "tp", None),
        P(),
        P(None, "tp"),
        P("tp", None),
        P("tp"),
        P(),
        P(),
        P(),
        P("ep", None, "tp"),
        P("ep", None, "tp"),
        P("ep", "tp", None),
    )
    return jax.shard_map(
        functools.partial(per_device, mesh.shape["ep"], mesh.shape["tp"]),
        mesh=mesh, in_specs=in_specs, out_specs=P("ep", "tp"), check_vma=False,
    )
```

```python
import functools

import jax
import jax.numpy as jnp
from jax import lax
from jax.experimental import pallas as pl
from jax.experimental.pallas import tpu as pltpu
from jax.sharding import PartitionSpec as P

GROUP_SIZE = 8
TOPK = 4
EPSILON = 1e-06
MESH = pl.DeviceIdType.MESH
BF = jnp.bfloat16
F32 = jnp.float32
KEY_CHUNKS = 4
NT = (((1,), (1,)), ((), ()))
TN = (((0,), (0,)), ((), ()))


def split3(values):
    first = values.astype(BF)
    rest = values - first.astype(F32)
    second = rest.astype(BF)
    third = (rest - second.astype(F32)).astype(BF)
    return first, second, third


def remote(src, dst, send, recv, device):
    return pltpu.make_async_remote_copy(
        src_ref=src, dst_ref=dst, send_sem=send, recv_sem=recv,
        device_id=device, device_id_type=MESH,
    )


def kernel(
    n_ep, n_tp, capacity,
    lens_ref, bias_ref, routes_ref, wexp_ref, wgrp_ref,
    mixg_hbm, moeg_hbm, res_hbm, wq_hbm, key_hbm, value_hbm, wo_hbm, wg_hbm, wu_hbm, wd_hbm,
    out_ref,
    mixg, moeg, res, wq, keys, values, wo, wg, wu, wd,
    qs, scores, sticks, att, head_send, head_recv, mid_all, slots, full,
    part_send, part_recv, pair_send, pair_recv, ret_send, ret_recv,
    small_sem, weight_sem, key_sem, value_sem,
    head_ss, head_rs, mid_ss, mid_rs, disp_ss, disp_rs,
    core_ss, core_rs, cross_ss, cross_rs, fwd_ss, fwd_rs,
    part_ss, part_rs, pair_ss, pair_rs, ret_ss, ret_rs,
):
    ep = lax.axis_index("ep")
    tp = lax.axis_index("tp")
    near = tp + 1 - 2 * (tp % 2)
    far = (tp + 2) % n_tp
    diag = (near + 2) % n_tp
    seqs, width = res.shape
    own = width // n_tp
    heads = bias_ref.shape[1]
    size = keys.shape[2]
    experts = wexp_ref.shape[0]

    def ep_peer(d):
        return lax.rem(ep + d, n_ep)

    def ep_source(d):
        return lax.rem(ep + n_ep - d, n_ep)

    loads = [
        pltpu.make_async_copy(src, dst, small_sem.at[i])
        for i, (src, dst) in enumerate(((res_hbm, res), (mixg_hbm, mixg), (moeg_hbm, moeg)))
    ]
    weights = [
        pltpu.make_async_copy(src, dst, weight_sem.at[i])
        for i, (src, dst) in enumerate(
            ((wq_hbm, wq), (wo_hbm, wo), (wg_hbm, wg), (wu_hbm, wu), (wd_hbm, wd))
        )
    ]
    step = seqs // KEY_CHUNKS
    key_loads = []
    value_loads = []
    for c in range(KEY_CHUNKS):
        rows = pl.ds(c * step, step)
        key_loads.append(pltpu.make_async_copy(key_hbm.at[rows], keys.at[rows], key_sem.at[c]))
        value_loads.append(
            pltpu.make_async_copy(value_hbm.at[rows], values.at[rows], value_sem.at[c])
        )
    for copy in loads + weights[:1]:
        copy.start()

    barrier = pltpu.get_barrier_semaphore()
    for d in range(1, n_tp):
        pl.semaphore_signal(
            barrier, inc=1, device_id={"tp": lax.rem(tp + d, n_tp)}, device_id_type=MESH
        )

    @pl.loop(1, n_ep)
    def _(d):
        pl.semaphore_signal(barrier, inc=1, device_id={"ep": ep_peer(d)}, device_id_type=MESH)

    for copy in loads:
        copy.wait()
    for copy in key_loads:
        copy.start()
    tokens = res[...].astype(F32)
    inverse = lax.rsqrt(jnp.sum(tokens * tokens, axis=1, keepdims=True) / width + EPSILON)
    normed = (tokens * inverse * mixg[...]).astype(BF)
    weights[0].wait()
    for copy in value_loads + weights[1:2]:
        copy.start()
    queries = jnp.dot(normed, wq[...], preferred_element_type=F32).astype(BF).astype(F32)
    for h in range(heads):
        qs[pl.ds(h, seqs, stride=heads), :] = queries[:, h * size:(h + 1) * size]
    per = 8 // heads
    row_of = lax.broadcasted_iota(jnp.int32, (8, 1), 0)
    for t in range(0, seqs, per):
        if t % step == 0:
            key_loads[t // step].wait()
        rows = qs[t * heads:t * heads + 8, :].astype(BF)
        total = None
        for j in range(per):
            term = lax.dot_general(rows, keys[t + j], NT, preferred_element_type=F32)
            total = term if total is None else jnp.where(row_of < j * heads, total, term)
        scores[t * heads:t * heads + 8, :] = total
    length = keys.shape[1]
    seq_of = lax.broadcasted_iota(jnp.int32, (seqs * heads, seqs), 0) // heads
    lens = jnp.sum(
        jnp.where(
            seq_of == lax.broadcasted_iota(jnp.int32, seq_of.shape, 1),
            lens_ref[...].astype(F32),
            0.0,
        ),
        axis=1,
        keepdims=True,
    )
    head_of = lax.broadcasted_iota(jnp.int32, (seqs * heads, heads), 0) % heads
    bias = jnp.sum(
        jnp.where(
            head_of == lax.broadcasted_iota(jnp.int32, head_of.shape, 1), bias_ref[...], 0.0
        ),
        axis=1,
        keepdims=True,
    )
    z = scores[...] * size ** (-0.5) + bias
    inside = lax.broadcasted_iota(jnp.int32, z.shape, 1).astype(F32) < lens
    low = jnp.log1p(jnp.exp(-jnp.abs(z)))
    remain = jnp.where(inside, -(jnp.maximum(z, 0.0) + low), 0.0)
    after = (
        lax.broadcasted_iota(jnp.int32, (length, length), 0)
        > lax.broadcasted_iota(jnp.int32, (length, length), 1)
    ).astype(F32).astype(BF)
    later = None
    for term in split3(remain):
        value = jnp.dot(term, after, preferred_element_type=F32)
        later = value if later is None else later + value
    sticks[...] = jnp.where(inside, jnp.exp(jnp.minimum(z, 0.0) - low + later), 0.0)
    for t in range(0, seqs, per):
        if t % step == 0:
            value_loads[t // step].wait()
        rows = sticks[t * heads:t * heads + 8, :].astype(BF)
        total = None
        for j in range(per):
            term = jnp.dot(rows, values[t + j], preferred_element_type=F32)
            total = term if total is None else jnp.where(row_of < j * heads, total, term)
        att[t * heads:t * heads + 8, :] = total
    attended = jnp.concatenate(
        [att[pl.ds(h, seqs, stride=heads), :].astype(BF) for h in range(heads)], axis=1
    )
    weights[1].wait()

    def head_block(p):
        columns = pl.ds(pl.multiple_of(p * own, own), own)
        return jnp.dot(attended, wo[:, columns], preferred_element_type=F32).astype(BF)

    pl.semaphore_wait(barrier, n_tp - 1 + n_ep - 1)
    head_copies = []
    for d, peer in ((1, diag), (2, far), (3, near)):
        head_send[peer] = head_block(peer)
        head_copies.append(
            remote(head_send.at[peer], head_recv.at[d], head_ss.at[d], head_rs.at[d], {"tp": peer})
        )
        head_copies[-1].start()
    for copy in weights[2:]:
        copy.start()

    routes = routes_ref[...]
    expert_row = lax.broadcasted_iota(jnp.int32, (experts, seqs), 0)
    chosen = jnp.zeros((experts, seqs), F32)
    for k in range(TOPK):
        chosen = chosen + jnp.where(routes[k:k + 1, :] == expert_row, 1.0, 0.0)
    before = (
        lax.broadcasted_iota(jnp.int32, (seqs, seqs), 0)
        < lax.broadcasted_iota(jnp.int32, (seqs, seqs), 1)
    ).astype(F32).astype(BF)
    earlier = jnp.dot(chosen.astype(BF), before, preferred_element_type=F32)
    slot_of = jnp.where(chosen > 0.5, earlier, -1.0)
    slot_row = lax.broadcasted_iota(jnp.int32, (experts, capacity, seqs), 1).astype(F32)
    place = jnp.where(
        jnp.broadcast_to(slot_of[:, None, :], slot_row.shape) == slot_row, 1.0, 0.0
    ).reshape(experts * capacity, seqs)

    attn = head_block(tp).astype(F32)
    for copy in head_copies:
        copy.wait_recv()
    for d in range(1, n_tp):
        attn = attn + head_recv[d].astype(F32)
    own_columns = pl.ds(pl.multiple_of(tp * own, own), own)
    mid_own = (
        res[:, own_columns].astype(F32) + attn.astype(BF).astype(F32)
    ).astype(BF)
    routed = jnp.dot(place.astype(BF), mid_own, preferred_element_type=F32).astype(BF)
    slots[...] = routed.reshape(experts, capacity, own)
    mid_all[tp] = mid_own

    def dispatch(d):
        return remote(
            slots.at[ep_peer(d)], full.at[tp, ep], disp_ss.at[d], disp_rs.at[d],
            {"ep": ep_peer(d)},
        )

    @pl.loop(1, n_ep)
    def _(d):
        dispatch(d).start()

    full[tp, ep] = slots[ep]
    mid_copies = []
    for d in range(1, n_tp):
        peer = lax.rem(tp + d, n_tp)
        mid_copies.append(
            remote(mid_all.at[tp], mid_all.at[tp], mid_ss.at[d], mid_rs.at[d], {"tp": peer})
        )
        mid_copies[-1].start()

    def to_core(d):
        at = (tp, ep_source(d))
        return remote(full.at[at], full.at[at], core_ss.at[d], core_rs.at[d], {"tp": near})

    def to_far(d):
        at = (tp, ep_source(d))
        return remote(full.at[at], full.at[at], cross_ss.at[d], cross_rs.at[d], {"tp": far})

    def onward(d):
        at = (far, ep_source(d))
        return remote(full.at[at], full.at[at], fwd_ss.at[d], fwd_rs.at[d], {"tp": near})

    to_far(0).start()
    to_core(0).start()

    @pl.loop(1, n_ep)
    def _(d):
        dispatch(d).wait_recv()
        to_far(d).start()
        to_core(d).start()

    @pl.loop(0, n_ep)
    def _(d):
        to_far(d).wait_recv()
        onward(d).start()

    for copy in weights[2:]:
        copy.wait()

    @pl.loop(0, n_ep)
    def _(d):
        to_core(d).wait_recv()

    @pl.loop(0, n_ep)
    def _(d):
        onward(d).wait_recv()

    rows = n_ep * capacity
    squares = jnp.zeros((rows, 1), F32)
    for p in range(n_tp):
        block = full[p].reshape(rows, own).astype(F32)
        squares = squares + jnp.sum(block * block, axis=1, keepdims=True)
    inverse = lax.rsqrt(squares / width + EPSILON)
    gate = None
    for p in range(n_tp):
        columns = slice(p * own, (p + 1) * own)
        block = full[p].reshape(rows, own).astype(F32)
        hidden = (block * inverse * moeg[:, columns]).astype(BF)
        gate_term = jnp.dot(hidden, wg[columns, :], preferred_element_type=F32)
        up_term = jnp.dot(hidden, wu[columns, :], preferred_element_type=F32)
        gate = gate_term if gate is None else gate + gate_term
        upward = up_term if p == 0 else upward + up_term
    active = (gate / (1.0 + jnp.exp(-gate)) * upward).astype(BF)

    def partial_of(p):
        columns = pl.ds(pl.multiple_of(p * own, own), own)
        value = jnp.dot(active, wd[:, columns], preferred_element_type=F32)
        return value.astype(BF).reshape(n_ep, capacity, own)

    part_copies = []
    for i, peer in enumerate((diag, near)):
        part_send[i] = partial_of(peer)
        part_copies.append(
            remote(part_send.at[i], part_recv.at[i], part_ss.at[i], part_rs.at[i], {"tp": near})
        )
        part_copies[-1].start()
    far_part = partial_of(far).astype(F32)
    part_copies[0].wait_recv()
    pair_send[...] = (far_part + part_recv[0].astype(F32)).astype(BF)

    def pair(d):
        at = ep_source(d)
        return remote(
            pair_send.at[at], pair_recv.at[at], pair_ss.at[d], pair_rs.at[d], {"tp": far}
        )

    @pl.loop(1, n_ep)
    def _(d):
        pair(d).start()

    pair(0).start()
    own_part = partial_of(tp).astype(F32)
    part_copies[1].wait_recv()
    ret_send[...] = own_part + part_recv[1].astype(F32)

    def giving(d):
        at = ep_source(d)
        return remote(slots.at[at], ret_recv.at[ep], ret_ss.at[d], ret_rs.at[d], {"ep": at})

    @pl.loop(1, n_ep)
    def _(d):
        dispatch(d).wait_send()

    @pl.loop(1, n_ep)
    def _(d):
        at = ep_source(d)
        pair(d).wait_recv()
        slots[at] = (ret_send[at] + pair_recv[at].astype(F32)).astype(BF)
        giving(d).start()

    pair(0).wait_recv()
    ret_recv[ep] = (ret_send[ep] + pair_recv[ep].astype(F32)).astype(BF)

    for copy in mid_copies:
        copy.wait_recv()
    squares = jnp.zeros((seqs, 1), F32)
    for p in range(n_tp):
        block = mid_all[p].astype(F32)
        squares = squares + jnp.sum(block * block, axis=1, keepdims=True)
    inverse = lax.rsqrt(squares / width + EPSILON)
    logit = jnp.zeros((experts, seqs), F32)
    group_logit = jnp.zeros((wgrp_ref.shape[0], seqs), F32)
    for p in range(n_tp):
        columns = slice(p * own, (p + 1) * own)
        hidden = (mid_all[p].astype(F32) * inverse * moeg[:, columns]).astype(BF)
        logit = logit + lax.dot_general(
            wexp_ref[:, columns], hidden, NT, preferred_element_type=F32
        )
        group_logit = group_logit + lax.dot_general(
            wgrp_ref[:, columns], hidden, NT, preferred_element_type=F32
        )
    group_exp = jnp.exp(group_logit - jnp.max(group_logit, axis=0, keepdims=True))
    group_prob = group_exp / jnp.sum(group_exp, axis=0, keepdims=True)
    group_row = lax.broadcasted_iota(jnp.int32, group_prob.shape, 0)
    group_of = jnp.zeros((1, seqs), jnp.int32) + lax.shift_right_logical(
        routes[0:1, :], jnp.full((1, seqs), GROUP_SIZE.bit_length() - 1, jnp.int32)
    )
    top_prob = jnp.sum(jnp.where(group_of == group_row, group_prob, 0.0), axis=0, keepdims=True)
    peak = jnp.max(jnp.where(chosen > 0.5, logit, -jnp.inf), axis=0, keepdims=True)
    raised = jnp.where(chosen > 0.5, jnp.exp(jnp.minimum(logit - peak, 0.0)), 0.0)
    share = raised / jnp.sum(raised, axis=0, keepdims=True) * top_prob
    combine = place * jnp.broadcast_to(share[:, None, :], slot_row.shape).reshape(place.shape)

    @pl.loop(1, n_ep)
    def _(d):
        remote(
            slots.at[ep], ret_recv.at[ep_peer(d)], ret_ss.at[d], ret_rs.at[d], {"ep": ep_source(d)}
        ).wait_recv()

    returned = ret_recv[...].reshape(experts * capacity, own)
    moe = None
    for term in split3(combine):
        value = lax.dot_general(term, returned, TN, preferred_element_type=F32)
        moe = value if moe is None else moe + value
    out_ref[...] = (mid_all[tp].astype(F32) + moe).astype(BF)

    for copy in head_copies + mid_copies + part_copies:
        copy.wait_send()

    @pl.loop(0, n_ep)
    def _(d):
        to_core(d).wait_send()
        to_far(d).wait_send()
        onward(d).wait_send()
        pair(d).wait_send()

    @pl.loop(1, n_ep)
    def _(d):
        giving(d).wait_send()


def per_device(
    n_ep, n_tp,
    residual, routes, lengths, key_cache, value_cache, mix_gain, w_query, w_out, head_bias,
    moe_gain, w_group, w_expert, expert_gate, expert_up, expert_down,
):
    seqs, width = residual.shape
    length, size = key_cache.shape[1], key_cache.shape[3]
    heads = head_bias.shape[0]
    experts, groups = w_expert.shape[1], w_group.shape[1]
    assert key_cache.shape[2] == 1 and expert_gate.shape[0] == 1 and n_tp == 4
    assert experts == n_ep
    own = width // n_tp
    units = expert_gate.shape[2]
    most = min(seqs, max(4, 2 * seqs // groups)) * TOPK // GROUP_SIZE
    capacity = -(-most // 16) * 16
    rows = seqs * heads
    vmem = pl.BlockSpec(memory_space=pltpu.VMEM)
    hbm = pl.BlockSpec(memory_space=pltpu.HBM)
    dma = pltpu.SemaphoreType.DMA
    return pl.pallas_call(
        functools.partial(kernel, n_ep, n_tp, capacity),
        out_shape=jax.ShapeDtypeStruct((seqs, own), BF),
        in_specs=[vmem] * 5 + [hbm] * 10,
        out_specs=vmem,
        scratch_shapes=[
            pltpu.VMEM((1, width), F32),
            pltpu.VMEM((1, width), F32),
            pltpu.VMEM((seqs, width), BF),
            pltpu.VMEM(w_query.shape, BF),
            pltpu.VMEM((seqs, length, size), BF),
            pltpu.VMEM((seqs, length, size), BF),
            pltpu.VMEM(w_out.shape, BF),
            pltpu.VMEM((width, units), BF),
            pltpu.VMEM((width, units), BF),
            pltpu.VMEM((units, width), BF),
            pltpu.VMEM((rows, size), F32),
            pltpu.VMEM((rows, length), F32),
            pltpu.VMEM((rows, length), F32),
            pltpu.VMEM((rows, size), F32),
            pltpu.VMEM((n_tp, seqs, own), BF),
            pltpu.VMEM((n_tp, seqs, own), BF),
            pltpu.VMEM((n_tp, seqs, own), BF),
            pltpu.VMEM((n_ep, capacity, own), BF),
            pltpu.VMEM((n_tp, n_ep, capacity, own), BF),
            pltpu.VMEM((2, n_ep, capacity, own), BF),
            pltpu.VMEM((2, n_ep, capacity, own), BF),
            pltpu.VMEM((n_ep, capacity, own), BF),
            pltpu.VMEM((n_ep, capacity, own), BF),
            pltpu.VMEM((n_ep, capacity, own), F32),
            pltpu.VMEM((n_ep, capacity, own), BF),
            dma((3,)), dma((5,)), dma((KEY_CHUNKS,)), dma((KEY_CHUNKS,)),
            dma((n_tp,)), dma((n_tp,)), dma((n_tp,)), dma((n_tp,)),
            dma((n_ep,)), dma((n_ep,)),
            dma((n_ep,)), dma((n_ep,)), dma((n_ep,)), dma((n_ep,)), dma((n_ep,)), dma((n_ep,)),
            dma((2,)), dma((2,)), dma((n_ep,)), dma((n_ep,)), dma((n_ep,)), dma((n_ep,)),
        ],
        compiler_params=pltpu.CompilerParams(
            collective_id=0, has_side_effects=True, vmem_limit_bytes=60 * 1024 * 1024
        ),
        name="decode_step",
    )(
        lengths.reshape(1, seqs),
        head_bias.reshape(1, heads),
        routes.T,
        w_expert.T,
        w_group.T,
        mix_gain.reshape(1, width),
        moe_gain.reshape(1, width),
        residual,
        w_query,
        key_cache.reshape(seqs, length, size),
        value_cache.reshape(seqs, length, size),
        w_out,
        expert_gate.reshape(width, units),
        expert_up.reshape(width, units),
        expert_down.reshape(units, width),
    )


def solution(mesh):
    in_specs = (
        P("ep", None),
        P("ep", None),
        P("ep"),
        P("ep", None, "tp", None),
        P("ep", None, "tp", None),
        P(),
        P(None, "tp"),
        P("tp", None),
        P("tp"),
        P(),
        P(),
        P(),
        P("ep", None, "tp"),
        P("ep", None, "tp"),
        P("ep", "tp", None),
    )
    return jax.shard_map(
        functools.partial(per_device, mesh.shape["ep"], mesh.shape["tp"]),
        mesh=mesh, in_specs=in_specs, out_specs=P("ep", "tp"), check_vma=False,
    )
```

```python
import functools

import jax
import jax.numpy as jnp
from jax import lax
from jax.experimental import pallas as pl
from jax.experimental.pallas import tpu as pltpu
from jax.sharding import PartitionSpec as P

GROUP_SIZE = 8
TOPK = 4
EPSILON = 1e-06
MESH = pl.DeviceIdType.MESH
BF = jnp.bfloat16
F32 = jnp.float32
KEY_CHUNKS = 4
NT = (((1,), (1,)), ((), ()))
TN = (((0,), (0,)), ((), ()))


def split3(values):
    first = values.astype(BF)
    rest = values - first.astype(F32)
    second = rest.astype(BF)
    third = (rest - second.astype(F32)).astype(BF)
    return first, second, third


def remote(src, dst, send, recv, device):
    return pltpu.make_async_remote_copy(
        src_ref=src, dst_ref=dst, send_sem=send, recv_sem=recv,
        device_id=device, device_id_type=MESH,
    )


def kernel(
    n_ep, n_tp, capacity,
    lens_ref, bias_ref, routes_ref, wexp_ref, wgrp_ref,
    mixg_hbm, moeg_hbm, res_hbm, wq_hbm, key_hbm, value_hbm, wo_hbm, wg_hbm, wu_hbm, wd_hbm,
    out_ref,
    mixg, moeg, res, wq, keys, values, wo, wg, wu, wd,
    qs, scores, sticks, att, head_send, head_recv, mid_all, slots, full,
    part_send, part_recv, pair_send, pair_recv, ret_send, ret_recv,
    small_sem, weight_sem, key_sem, value_sem,
    head_ss, head_rs, mid_ss, mid_rs, disp_ss, disp_rs,
    core_ss, core_rs, cross_ss, cross_rs, fwd_ss, fwd_rs,
    part_ss, part_rs, pair_ss, pair_rs, ret_ss, ret_rs,
):
    ep = lax.axis_index("ep")
    tp = lax.axis_index("tp")
    near = tp + 1 - 2 * (tp % 2)
    far = (tp + 2) % n_tp
    diag = (near + 2) % n_tp
    seqs, width = res.shape
    own = width // n_tp
    heads = bias_ref.shape[1]
    size = keys.shape[2]
    experts = wexp_ref.shape[0]

    def ep_peer(d):
        peer, bit = 0, 1
        while bit < n_ep:
            peer = peer + (ep // bit + d // bit) % 2 * bit
            bit *= 2
        return peer

    loads = [
        pltpu.make_async_copy(src, dst, small_sem.at[i])
        for i, (src, dst) in enumerate(((res_hbm, res), (mixg_hbm, mixg), (moeg_hbm, moeg)))
    ]
    top, end = pl.ds(0, width // 2), pl.ds(width // 2, width // 2)
    weights = [
        pltpu.make_async_copy(src, dst, weight_sem.at[i])
        for i, (src, dst) in enumerate(
            ((wq_hbm.at[top], wq.at[top]), (wq_hbm.at[end], wq.at[end]), (wo_hbm, wo), (wg_hbm, wg), (wu_hbm, wu), (wd_hbm, wd))
        )
    ]
    step = seqs // KEY_CHUNKS
    key_loads = []
    value_loads = []
    for c in range(KEY_CHUNKS):
        rows = pl.ds(c * step, step)
        key_loads.append(pltpu.make_async_copy(key_hbm.at[rows], keys.at[rows], key_sem.at[c]))
        value_loads.append(
            pltpu.make_async_copy(value_hbm.at[rows], values.at[rows], value_sem.at[c])
        )
    for copy in loads + weights[:2]:
        copy.start()

    barrier = pltpu.get_barrier_semaphore()
    for d in range(1, n_tp):
        pl.semaphore_signal(
            barrier, inc=1, device_id={"tp": lax.rem(tp + d, n_tp)}, device_id_type=MESH
        )

    @pl.loop(1, n_ep)
    def _(d):
        pl.semaphore_signal(barrier, inc=1, device_id={"ep": ep_peer(d)}, device_id_type=MESH)

    for copy in loads:
        copy.wait()
    for copy in key_loads:
        copy.start()
    tokens = res[...].astype(F32)
    inverse = lax.rsqrt(jnp.sum(tokens * tokens, axis=1, keepdims=True) / width + EPSILON)
    normed = (tokens * inverse * mixg[...]).astype(BF)
    weights[0].wait()
    queries = jnp.dot(normed[:, :width // 2], wq[top, :], preferred_element_type=F32)
    weights[1].wait()
    for copy in value_loads + weights[2:3]:
        copy.start()
    queries = queries + jnp.dot(normed[:, width // 2:], wq[end, :], preferred_element_type=F32)
    queries = queries.astype(BF).astype(F32)
    for h in range(heads):
        qs[pl.ds(h, seqs, stride=heads), :] = queries[:, h * size:(h + 1) * size]
    per = 8 // heads
    row_of = lax.broadcasted_iota(jnp.int32, (8, 1), 0)
    for t in range(0, seqs, per):
        if t % step == 0:
            key_loads[t // step].wait()
        rows = qs[t * heads:t * heads + 8, :].astype(BF)
        total = None
        for j in range(per):
            term = lax.dot_general(rows, keys[t + j], NT, preferred_element_type=F32)
            total = term if total is None else jnp.where(row_of < j * heads, total, term)
        scores[t * heads:t * heads + 8, :] = total
    length = keys.shape[1]
    seq_of = lax.broadcasted_iota(jnp.int32, (seqs * heads, seqs), 0) // heads
    lens = jnp.sum(
        jnp.where(
            seq_of == lax.broadcasted_iota(jnp.int32, seq_of.shape, 1),
            lens_ref[...].astype(F32),
            0.0,
        ),
        axis=1,
        keepdims=True,
    )
    head_of = lax.broadcasted_iota(jnp.int32, (seqs * heads, heads), 0) % heads
    bias = jnp.sum(
        jnp.where(
            head_of == lax.broadcasted_iota(jnp.int32, head_of.shape, 1), bias_ref[...], 0.0
        ),
        axis=1,
        keepdims=True,
    )
    z = scores[...] * size ** (-0.5) + bias
    inside = lax.broadcasted_iota(jnp.int32, z.shape, 1).astype(F32) < lens
    low = jnp.log1p(jnp.exp(-jnp.abs(z)))
    remain = jnp.where(inside, -(jnp.maximum(z, 0.0) + low), 0.0)
    after = (
        lax.broadcasted_iota(jnp.int32, (length, length), 0)
        > lax.broadcasted_iota(jnp.int32, (length, length), 1)
    ).astype(F32).astype(BF)
    later = None
    for term in split3(remain):
        value = jnp.dot(term, after, preferred_element_type=F32)
        later = value if later is None else later + value
    sticks[...] = jnp.where(inside, jnp.exp(jnp.minimum(z, 0.0) - low + later), 0.0)
    for t in range(0, seqs, per):
        if t % step == 0:
            value_loads[t // step].wait()
        rows = sticks[t * heads:t * heads + 8, :].astype(BF)
        total = None
        for j in range(per):
            term = jnp.dot(rows, values[t + j], preferred_element_type=F32)
            total = term if total is None else jnp.where(row_of < j * heads, total, term)
        att[t * heads:t * heads + 8, :] = total
    attended = jnp.concatenate(
        [att[pl.ds(h, seqs, stride=heads), :].astype(BF) for h in range(heads)], axis=1
    )
    weights[2].wait()

    def head_block(p):
        columns = pl.ds(pl.multiple_of(p * own, own), own)
        return jnp.dot(attended, wo[:, columns], preferred_element_type=F32).astype(BF)

    pl.semaphore_wait(barrier, n_tp - 1 + n_ep - 1)
    head_copies = []
    for d, peer in ((1, diag), (2, far), (3, near)):
        head_send[peer] = head_block(peer)
        head_copies.append(
            remote(head_send.at[peer], head_recv.at[d], head_ss.at[d], head_rs.at[d], {"tp": peer})
        )
        head_copies[-1].start()
    for copy in weights[3:]:
        copy.start()

    routes = routes_ref[...]
    expert_row = lax.broadcasted_iota(jnp.int32, (experts, seqs), 0)
    chosen = jnp.zeros((experts, seqs), F32)
    for k in range(TOPK):
        chosen = chosen + jnp.where(routes[k:k + 1, :] == expert_row, 1.0, 0.0)
    before = (
        lax.broadcasted_iota(jnp.int32, (seqs, seqs), 0)
        < lax.broadcasted_iota(jnp.int32, (seqs, seqs), 1)
    ).astype(F32).astype(BF)
    earlier = jnp.dot(chosen.astype(BF), before, preferred_element_type=F32)
    slot_of = jnp.where(chosen > 0.5, earlier, -1.0)
    slot_row = lax.broadcasted_iota(jnp.int32, (experts, capacity, seqs), 1).astype(F32)
    place = jnp.where(
        jnp.broadcast_to(slot_of[:, None, :], slot_row.shape) == slot_row, 1.0, 0.0
    ).reshape(experts * capacity, seqs)

    attn = head_block(tp).astype(F32)
    for copy in head_copies:
        copy.wait_recv()
    for d in range(1, n_tp):
        attn = attn + head_recv[d].astype(F32)
    own_columns = pl.ds(pl.multiple_of(tp * own, own), own)
    mid_own = (
        res[:, own_columns].astype(F32) + attn.astype(BF).astype(F32)
    ).astype(BF)
    routed = jnp.dot(place.astype(BF), mid_own, preferred_element_type=F32).astype(BF)
    slots[...] = routed.reshape(experts, capacity, own)
    mid_all[tp] = mid_own

    def dispatch(d):
        return remote(
            slots.at[ep_peer(d)], full.at[tp, ep], disp_ss.at[d], disp_rs.at[d],
            {"ep": ep_peer(d)},
        )

    @pl.loop(1, n_ep)
    def _(d):
        dispatch(n_ep - d).start()

    full[tp, ep] = slots[ep]
    mid_copies = []
    for d in range(1, n_tp):
        peer = lax.rem(tp + d, n_tp)
        mid_copies.append(
            remote(mid_all.at[tp], mid_all.at[tp], mid_ss.at[d], mid_rs.at[d], {"tp": peer})
        )
        mid_copies[-1].start()

    def to_core(d):
        at = (tp, ep_peer(d))
        return remote(full.at[at], full.at[at], core_ss.at[d], core_rs.at[d], {"tp": near})

    def to_far(d):
        at = (tp, ep_peer(d))
        return remote(full.at[at], full.at[at], cross_ss.at[d], cross_rs.at[d], {"tp": far})

    def onward(d):
        at = (far, ep_peer(d))
        return remote(full.at[at], full.at[at], fwd_ss.at[d], fwd_rs.at[d], {"tp": near})

    to_far(0).start()
    to_core(0).start()

    @pl.loop(1, n_ep)
    def _(d):
        dispatch(d).wait_recv()
        to_far(d).start()
        to_core(d).start()

    @pl.loop(0, n_ep)
    def _(d):
        to_far(d).wait_recv()
        onward(d).start()

    for copy in weights[3:]:
        copy.wait()

    @pl.loop(0, n_ep)
    def _(d):
        to_core(d).wait_recv()

    @pl.loop(0, n_ep)
    def _(d):
        onward(d).wait_recv()

    rows = n_ep * capacity
    squares = jnp.zeros((rows, 1), F32)
    for p in range(n_tp):
        block = full[p].reshape(rows, own).astype(F32)
        squares = squares + jnp.sum(block * block, axis=1, keepdims=True)
    inverse = lax.rsqrt(squares / width + EPSILON)
    gate = None
    for p in range(n_tp):
        columns = slice(p * own, (p + 1) * own)
        block = full[p].reshape(rows, own).astype(F32)
        hidden = (block * inverse * moeg[:, columns]).astype(BF)
        gate_term = jnp.dot(hidden, wg[columns, :], preferred_element_type=F32)
        up_term = jnp.dot(hidden, wu[columns, :], preferred_element_type=F32)
        gate = gate_term if gate is None else gate + gate_term
        upward = up_term if p == 0 else upward + up_term
    active = (gate / (1.0 + jnp.exp(-gate)) * upward).astype(BF)

    def partial_of(p):
        columns = pl.ds(pl.multiple_of(p * own, own), own)
        value = jnp.dot(active, wd[:, columns], preferred_element_type=F32)
        return value.astype(BF).reshape(n_ep, capacity, own)

    part_copies = []
    for i, peer in enumerate((diag, near)):
        part_send[i] = partial_of(peer)
        part_copies.append(
            remote(part_send.at[i], part_recv.at[i], part_ss.at[i], part_rs.at[i], {"tp": near})
        )
        part_copies[-1].start()
    far_part = partial_of(far).astype(F32)
    part_copies[0].wait_recv()
    pair_send[...] = (far_part + part_recv[0].astype(F32)).astype(BF)

    def pair(d):
        at = ep_peer(d)
        return remote(
            pair_send.at[at], pair_recv.at[at], pair_ss.at[d], pair_rs.at[d], {"tp": far}
        )

    @pl.loop(1, n_ep)
    def _(d):
        pair(n_ep - d).start()

    pair(0).start()
    own_part = partial_of(tp).astype(F32)
    part_copies[1].wait_recv()
    ret_send[...] = own_part + part_recv[1].astype(F32)

    def giving(d):
        at = ep_peer(d)
        return remote(slots.at[at], ret_recv.at[ep], ret_ss.at[d], ret_rs.at[d], {"ep": at})

    @pl.loop(1, n_ep)
    def _(d):
        dispatch(d).wait_send()

    @pl.loop(1, n_ep)
    def _(i):
        d = n_ep - i
        at = ep_peer(d)
        pair(d).wait_recv()
        slots[at] = (ret_send[at] + pair_recv[at].astype(F32)).astype(BF)
        giving(d).start()

    pair(0).wait_recv()
    ret_recv[ep] = (ret_send[ep] + pair_recv[ep].astype(F32)).astype(BF)

    for copy in mid_copies:
        copy.wait_recv()
    squares = jnp.zeros((seqs, 1), F32)
    for p in range(n_tp):
        block = mid_all[p].astype(F32)
        squares = squares + jnp.sum(block * block, axis=1, keepdims=True)
    inverse = lax.rsqrt(squares / width + EPSILON)
    logit = jnp.zeros((experts, seqs), F32)
    group_logit = jnp.zeros((wgrp_ref.shape[0], seqs), F32)
    for p in range(n_tp):
        columns = slice(p * own, (p + 1) * own)
        hidden = (mid_all[p].astype(F32) * inverse * moeg[:, columns]).astype(BF)
        logit = logit + lax.dot_general(
            wexp_ref[:, columns], hidden, NT, preferred_element_type=F32
        )
        group_logit = group_logit + lax.dot_general(
            wgrp_ref[:, columns], hidden, NT, preferred_element_type=F32
        )
    group_exp = jnp.exp(group_logit - jnp.max(group_logit, axis=0, keepdims=True))
    group_prob = group_exp / jnp.sum(group_exp, axis=0, keepdims=True)
    group_row = lax.broadcasted_iota(jnp.int32, group_prob.shape, 0)
    group_of = jnp.zeros((1, seqs), jnp.int32) + lax.shift_right_logical(
        routes[0:1, :], jnp.full((1, seqs), GROUP_SIZE.bit_length() - 1, jnp.int32)
    )
    top_prob = jnp.sum(jnp.where(group_of == group_row, group_prob, 0.0), axis=0, keepdims=True)
    peak = jnp.max(jnp.where(chosen > 0.5, logit, -jnp.inf), axis=0, keepdims=True)
    raised = jnp.where(chosen > 0.5, jnp.exp(jnp.minimum(logit - peak, 0.0)), 0.0)
    share = raised / jnp.sum(raised, axis=0, keepdims=True) * top_prob
    combine = place * jnp.broadcast_to(share[:, None, :], slot_row.shape).reshape(place.shape)

    @pl.loop(1, n_ep)
    def _(d):
        remote(
            slots.at[ep], ret_recv.at[ep_peer(d)], ret_ss.at[d], ret_rs.at[d], {"ep": ep_peer(d)}
        ).wait_recv()

    returned = ret_recv[...].reshape(experts * capacity, own)
    moe = None
    for term in split3(combine):
        value = lax.dot_general(term, returned, TN, preferred_element_type=F32)
        moe = value if moe is None else moe + value
    out_ref[...] = (mid_all[tp].astype(F32) + moe).astype(BF)

    for copy in head_copies + mid_copies + part_copies:
        copy.wait_send()

    @pl.loop(0, n_ep)
    def _(d):
        to_core(d).wait_send()
        to_far(d).wait_send()
        onward(d).wait_send()
        pair(d).wait_send()

    @pl.loop(1, n_ep)
    def _(d):
        giving(d).wait_send()


def per_device(
    n_ep, n_tp,
    residual, routes, lengths, key_cache, value_cache, mix_gain, w_query, w_out, head_bias,
    moe_gain, w_group, w_expert, expert_gate, expert_up, expert_down,
):
    seqs, width = residual.shape
    length, size = key_cache.shape[1], key_cache.shape[3]
    heads = head_bias.shape[0]
    experts, groups = w_expert.shape[1], w_group.shape[1]
    assert key_cache.shape[2] == 1 and expert_gate.shape[0] == 1 and n_tp == 4
    assert experts == n_ep
    own = width // n_tp
    units = expert_gate.shape[2]
    most = min(seqs, max(4, 2 * seqs // groups)) * TOPK // GROUP_SIZE
    capacity = -(-most // 16) * 16
    rows = seqs * heads
    vmem = pl.BlockSpec(memory_space=pltpu.VMEM)
    hbm = pl.BlockSpec(memory_space=pltpu.HBM)
    dma = pltpu.SemaphoreType.DMA
    return pl.pallas_call(
        functools.partial(kernel, n_ep, n_tp, capacity),
        out_shape=jax.ShapeDtypeStruct((seqs, own), BF),
        in_specs=[vmem] * 5 + [hbm] * 10,
        out_specs=vmem,
        scratch_shapes=[
            pltpu.VMEM((1, width), F32),
            pltpu.VMEM((1, width), F32),
            pltpu.VMEM((seqs, width), BF),
            pltpu.VMEM(w_query.shape, BF),
            pltpu.VMEM((seqs, length, size), BF),
            pltpu.VMEM((seqs, length, size), BF),
            pltpu.VMEM(w_out.shape, BF),
            pltpu.VMEM((width, units), BF),
            pltpu.VMEM((width, units), BF),
            pltpu.VMEM((units, width), BF),
            pltpu.VMEM((rows, size), F32),
            pltpu.VMEM((rows, length), F32),
            pltpu.VMEM((rows, length), F32),
            pltpu.VMEM((rows, size), F32),
            pltpu.VMEM((n_tp, seqs, own), BF),
            pltpu.VMEM((n_tp, seqs, own), BF),
            pltpu.VMEM((n_tp, seqs, own), BF),
            pltpu.VMEM((n_ep, capacity, own), BF),
            pltpu.VMEM((n_tp, n_ep, capacity, own), BF),
            pltpu.VMEM((2, n_ep, capacity, own), BF),
            pltpu.VMEM((2, n_ep, capacity, own), BF),
            pltpu.VMEM((n_ep, capacity, own), BF),
            pltpu.VMEM((n_ep, capacity, own), BF),
            pltpu.VMEM((n_ep, capacity, own), F32),
            pltpu.VMEM((n_ep, capacity, own), BF),
            dma((3,)), dma((6,)), dma((KEY_CHUNKS,)), dma((KEY_CHUNKS,)),
            dma((n_tp,)), dma((n_tp,)), dma((n_tp,)), dma((n_tp,)),
            dma((n_ep,)), dma((n_ep,)),
            dma((n_ep,)), dma((n_ep,)), dma((n_ep,)), dma((n_ep,)), dma((n_ep,)), dma((n_ep,)),
            dma((2,)), dma((2,)), dma((n_ep,)), dma((n_ep,)), dma((n_ep,)), dma((n_ep,)),
        ],
        compiler_params=pltpu.CompilerParams(
            collective_id=0, has_side_effects=True, vmem_limit_bytes=60 * 1024 * 1024
        ),
        name="decode_step",
    )(
        lengths.reshape(1, seqs),
        head_bias.reshape(1, heads),
        routes.T,
        w_expert.T,
        w_group.T,
        mix_gain.reshape(1, width),
        moe_gain.reshape(1, width),
        residual,
        w_query,
        key_cache.reshape(seqs, length, size),
        value_cache.reshape(seqs, length, size),
        w_out,
        expert_gate.reshape(width, units),
        expert_up.reshape(width, units),
        expert_down.reshape(units, width),
    )


def solution(mesh):
    in_specs = (
        P("ep", None),
        P("ep", None),
        P("ep"),
        P("ep", None, "tp", None),
        P("ep", None, "tp", None),
        P(),
        P(None, "tp"),
        P("tp", None),
        P("tp"),
        P(),
        P(),
        P(),
        P("ep", None, "tp"),
        P("ep", None, "tp"),
        P("ep", "tp", None),
    )
    return jax.shard_map(
        functools.partial(per_device, mesh.shape["ep"], mesh.shape["tp"]),
        mesh=mesh, in_specs=in_specs, out_specs=P("ep", "tp"), check_vma=False,
    )
```
